768 devices in a mesh: sp: 16 (over y, core), dp: 48 (over z, x).
Axes of the slice: x: 4, y: 8, z: 12, core: 2. Of those that a mesh axis runs over, the one named last changes fastest.
Arguments:
- q_latent: bfloat16 [48, 2048, 512], P('dp', 'sp'), may hold values from -70 to 70
- kv_latent: bfloat16 [48, 2048, 512], P('dp', 'sp'), may hold values from -70 to 70
- rope_key: bfloat16 [48, 2048, 64], P('dp', 'sp'), may hold values from -370 to 370
- w_query: bfloat16 [512, 3072], P(None, 'dp'), may hold values from -0.25 to 0.25
- w_keyval: bfloat16 [512, 4096], P(None, 'sp'), may hold values from -0.25 to 0.25
- w_out: bfloat16 [2048, 2048], replicated, may hold values from -0.125 to 0.125
- query_gain: bfloat16 [512], replicated, may hold values from 0.099609375 to 1.8984375
- latent_gain: bfloat16 [512], replicated, may hold values from 0.099609375 to 1.8984375
- out_gain: bfloat16 [2048], replicated, may hold values from 0.099609375 to 1.8984375
Outputs:
- output: bfloat16 [48, 2048, 2048], P('dp', 'sp')
The draws below stay inside these ranges and needn't reach their ends.
All inputs are finite; a program needn't handle non-finite values.
Results may differ from the reference program's by a relative error of at most 0.03.
The reference program's roundings to bfloat16 on the way (of `query_norm`, `queries`, `latent_norm`, `keyval`, `rope_turned`, `weights`, `attended` and `mixed_norm`) count: a program that leaves them out, or rounds other values in their place, can miss the bound.
Values may be sent and summed in bfloat16 or wider, within the bound.
A program may use at most 64 MiB of HBM per device.

```python
import math
import jax
import jax.numpy as jnp
from jax import lax

D = 2048
H = 16
QR = 512
KR = 512
NOPE = 128
ROPE = 64
VDIM = 128
SEQ_LEN = 2048
SEQS = 48


def scaled_latent_draw(key, width):
    base_key, channel_key, row_key = jax.random.split(key, 3)
    array_shape = (SEQS, SEQ_LEN, width)
    base_draw = jnp.clip(jax.random.normal(base_key, array_shape, jnp.float32), -5.0, 5.0)
    channel = jnp.exp(jax.random.uniform(channel_key, (width,), jnp.float32, math.log(0.3), math.log(3.0)))
    row_scale = jnp.exp(jax.random.uniform(row_key, (SEQS, SEQ_LEN, 1), jnp.float32, math.log(0.3), math.log(3.0)))
    return base_draw * channel * row_scale


def draw_q_latent(key, part):
    return scaled_latent_draw(jax.random.fold_in(key, 11), QR).astype(jnp.bfloat16)


def draw_kv_latent(key, part):
    return scaled_latent_draw(jax.random.fold_in(key, 12), KR).astype(jnp.bfloat16)


def draw_rope_key(key, part):
    base_key = jax.random.fold_in(jax.random.fold_in(key, 13), 0)
    array_shape = (SEQS, SEQ_LEN, ROPE)
    result_draw = jnp.clip(jax.random.normal(base_key, array_shape, jnp.float32), -5.0, 5.0)
    return result_draw.astype(jnp.bfloat16)


def steps_of(own_key, extent, cuts, least, largest):
    gain = 1.0
    for dim, parts in cuts:
        draws = jax.random.uniform(jax.random.fold_in(jax.random.fold_in(own_key, 6), dim), (parts,), jnp.float32, least / len(cuts), largest / len(cuts))
        gain = gain * jnp.repeat(jnp.exp(draws), extent[dim] // parts).reshape((-1,) + (1,) * (len(extent) - 1 - dim))
    return gain


def noise(own_key, shape, scale, limit, cuts=(), kind=jnp.bfloat16):
    values = scale * jax.random.normal(own_key, shape, jnp.float32)
    if cuts:
        values = values * steps_of(own_key, shape, cuts, -0.22, 0.18)
    return jnp.clip(values, -limit, limit).astype(kind)


def setup_inputs(seed: int = 0) -> dict:
    keys = jax.random.split(jax.random.key(seed), 10)
    return {
        "q_latent": draw_q_latent(jax.random.fold_in(keys[9], 71), 0),
        "kv_latent": draw_kv_latent(jax.random.fold_in(keys[9], 71), 0),
        "rope_key": draw_rope_key(jax.random.fold_in(keys[9], 71), 0),
        "w_query": noise(keys[3], (QR, H * (NOPE + ROPE)), QR ** -0.5, 0.25, ((1, 48),)),
        "w_keyval": noise(keys[4], (KR, H * (NOPE + VDIM)), KR ** -0.5, 0.25, ((1, 16),)),
        "w_out": noise(keys[5], (H * VDIM, D), (H * VDIM) ** -0.5, 0.125),
        "query_gain": jnp.clip(1.0 + 0.18 * jax.random.normal(keys[6], (QR,), jnp.float32), 0.099609375, 1.8984375).astype(jnp.bfloat16),
        "latent_gain": jnp.clip(1.0 + 0.18 * jax.random.normal(keys[7], (KR,), jnp.float32), 0.099609375, 1.8984375).astype(jnp.bfloat16),
        "out_gain": jnp.clip(1.0 + 0.18 * jax.random.normal(keys[8], (H * VDIM,), jnp.float32), 0.099609375, 1.8984375).astype(jnp.bfloat16),
    }


def normalize(row_values, gain_vector):
    widened = row_values.astype(jnp.float32)
    return widened * lax.rsqrt(lax.optimization_barrier(jnp.mean(widened * widened, axis=-1, keepdims=True)) + 1e-05) * gain_vector.astype(jnp.float32)

def angles_for(positions, rope_width):
    half_width = rope_width // 2
    inverse = 10000.0 ** (-jnp.arange(half_width, dtype=jnp.float32) / half_width)
    return positions.astype(jnp.float32)[:, None] * inverse[None, :]

def turn(vectors, angles):
    half_width = vectors.shape[-1] // 2
    cosine = jnp.cos(angles)
    sine_value = jnp.sin(angles)
    low_half = vectors[..., :half_width]
    high_half = vectors[..., half_width:]
    return jnp.concatenate([low_half * cosine - high_half * sine_value, high_half * cosine + low_half * sine_value], axis=-1)

def one_sequence(query_latent, kv_rows, rope_rows, w_query, w_keyval, w_out, query_gain, latent_gain, out_gain):
    length = query_latent.shape[0]
    positions = jnp.arange(length, dtype=jnp.int32)
    angles = angles_for(positions, ROPE)
    query_norm = normalize(query_latent, query_gain).astype(jnp.bfloat16)
    query_raw = jnp.dot(query_norm, w_query, preferred_element_type=jnp.float32).reshape(length, H, NOPE + ROPE)
    queries = jnp.concatenate([query_raw[..., :NOPE], turn(query_raw[..., NOPE:], angles[:, None, :])], axis=-1).astype(jnp.bfloat16)
    queries = lax.optimization_barrier(queries)
    latent_norm = normalize(kv_rows, latent_gain).astype(jnp.bfloat16)
    keyval = jnp.dot(latent_norm, w_keyval, preferred_element_type=jnp.float32).astype(jnp.bfloat16)
    keyval = lax.optimization_barrier(keyval).reshape(length, H, NOPE + VDIM)
    rope_turned = turn(rope_rows.astype(jnp.float32), angles).astype(jnp.bfloat16)
    rope_turned = lax.optimization_barrier(rope_turned)
    key_rows = jnp.concatenate([keyval[..., :NOPE], jnp.broadcast_to(rope_turned[:, None, :], (length, H, ROPE))], axis=-1)
    value_rows = keyval[..., NOPE:]
    block_rows = min(512, length)
    score_scale = (NOPE + ROPE) ** (-0.5)
    pieces = []
    for block_index in range(length // block_rows):
        block_start = block_index * block_rows
        block_stop = block_start + block_rows
        scores = jnp.einsum('qhd,khd->hqk', queries[block_start:block_stop].astype(jnp.float32), key_rows[:block_stop].astype(jnp.float32)) * score_scale
        allowed = jnp.arange(block_stop)[None, :] <= (block_start + jnp.arange(block_rows))[:, None]
        scores = jnp.where(allowed[None], scores, -jnp.inf)
        row_top = lax.optimization_barrier(jnp.max(scores, axis=-1, keepdims=True))
        exponent = jnp.exp(scores - row_top)
        row_total = lax.optimization_barrier(jnp.sum(exponent, axis=-1))
        weights = lax.optimization_barrier(exponent.astype(jnp.bfloat16))
        summed = jnp.einsum('hqk,khd->qhd', weights.astype(jnp.float32), value_rows[:block_stop].astype(jnp.float32))
        pieces.append((summed / jnp.transpose(row_total)[:, :, None]).astype(jnp.bfloat16))
    attended = lax.optimization_barrier(jnp.concatenate(pieces, axis=0)).reshape(length, H * VDIM)
    mixed_norm = normalize(attended, out_gain).astype(jnp.bfloat16)
    return jnp.dot(mixed_norm, w_out, preferred_element_type=jnp.float32).astype(jnp.bfloat16)

def reference(q_latent, kv_latent, rope_key, w_query, w_keyval, w_out, query_gain, latent_gain, out_gain):

    def per_sequence(inputs):
        return one_sequence(inputs[0], inputs[1], inputs[2], w_query, w_keyval, w_out, query_gain, latent_gain, out_gain)
    return lax.map(per_sequence, (q_latent, kv_latent, rope_key))
```

```python
import functools
import math

import jax
import jax.numpy as jnp
import numpy as np
from jax import lax
from jax.experimental import pallas as pl
from jax.experimental.pallas import tpu as pltpu
from jax.sharding import PartitionSpec as P

H = 16
NOPE = 128
ROPE = 64
VDIM = 128
D = 2048
SP = 16
CHIPS = SP // 2
NX = 4
ROWS = 128
LAT = 512
KV_ROWS = 144
MSG_ROWS = KV_ROWS + ROWS
CUT = 80
EPS = 1e-05
EXPONENT = (NOPE + ROPE) ** (-0.5) * math.log2(math.e)
BF16 = jnp.bfloat16
F32 = jnp.float32
MESH = pl.DeviceIdType.MESH


def rotary_tables():
    inverse = np.float32(10000.0) ** (-np.arange(32, dtype=np.float32) / np.float32(32))

    def both(positions):
        angles = positions.astype(np.float64)[:, None] * inverse.astype(np.float64)[None, :]
        return np.cos(angles), np.sin(angles)

    far_cos, far_sin = both(np.arange(SP) * ROWS)
    near_cos, near_sin = both(np.arange(ROWS))
    u = np.concatenate([far_cos, far_cos, -far_sin, far_sin], axis=1)
    v = np.concatenate([-far_sin, -far_sin, -far_cos, far_cos], axis=1)
    c = np.concatenate([near_cos] * 4, axis=1)
    s = np.concatenate([near_sin] * 4, axis=1)
    return np.concatenate([u, v, c, s], axis=0).astype(np.float32)


def selection(shape, pairs):
    row = lax.broadcasted_iota(jnp.int32, shape, 0)
    column = lax.broadcasted_iota(jnp.int32, shape, 1)
    hit = None
    for row_from, column_from, width in pairs:
        here = (
            (column >= column_from)
            & (column < column_from + width)
            & (column - column_from == row - row_from)
        )
        hit = here if hit is None else hit | here
    return jnp.where(hit, 1.0, 0.0).astype(BF16)


def dot(a, b):
    return jnp.dot(a, b, preferred_element_type=F32)


def normalized(x, gain):
    wide = x.astype(F32)
    mean = jnp.mean(wide * wide, axis=-1, keepdims=True)
    return (wide * lax.rsqrt(mean + EPS) * gain.astype(F32)).astype(BF16)


def kernel(
    nz,
    q_in,
    kv_in,
    rope_in,
    wq_in,
    wkv_in,
    wout_in,
    qg_ref,
    lg_ref,
    og_ref,
    tab_in,
    out_ref,
    xq,
    xkv,
    xr,
    xw,
    wkv,
    wout,
    tab,
    msg,
    ws,
    wext,
    kx,
    vx,
    att,
    rcv,
    acc,
    outv,
    ogain,
    load_sem,
    ring_send,
    ring_recv,
    sib_send,
    sib_recv,
    ret_send,
    ret_recv,
    wz_send,
    wx_send,
    w_recv,
):
    s = lax.axis_index("sp")
    y = s // 2
    sib = s + 1 - 2 * lax.rem(s, 2)
    right = lax.rem(s + 2, SP)
    left = lax.rem(s + SP - 2, SP)
    spread = nz > 1
    if spread:
        dp = lax.axis_index("dp")
        z = dp // NX
        x = lax.rem(dp, NX)

    barrier = pltpu.get_barrier_semaphore()
    greeted = 0
    for step in range(1, SP):
        pl.semaphore_signal(
            barrier, inc=1, device_id={"sp": lax.rem(s + step, SP)}, device_id_type=MESH
        )
        greeted += 1
    if spread:
        for step in range(1, nz):
            pl.semaphore_signal(
                barrier,
                inc=1,
                device_id={"dp": lax.rem(z + step, nz) * NX + x},
                device_id_type=MESH,
            )
            greeted += 1
        for step in range(1, NX):
            pl.semaphore_signal(
                barrier,
                inc=1,
                device_id={"dp": z * NX + lax.rem(x + step, NX)},
                device_id_type=MESH,
            )
            greeted += 1

    loads = [
        pltpu.make_async_copy(source, target, load_sem.at[i])
        for i, (source, target) in enumerate(
            [
                (kv_in, xkv),
                (rope_in, xr),
                (tab_in, tab),
                (q_in, xq),
                (wq_in, xw),
                (wkv_in, wkv),
                (wout_in, wout),
            ]
        )
    ]
    for load in loads:
        load.start()

    def turning(slot):
        return (
            tab[pl.ds(slot, 1), :] * tab[2 * SP : 2 * SP + ROWS, :]
            + tab[pl.ds(SP + slot, 1), :] * tab[2 * SP + ROWS :, :]
        )

    def turned(halves, slot):
        products = halves * turning(slot)
        return products + pltpu.roll(products, 64, 1)

    low_lanes = lax.broadcasted_iota(jnp.int32, (ROWS // 2, 128), 1) < 64

    loads[0].wait()
    msg[s, 0:ROWS, :] = normalized(xkv[...], lg_ref[...])
    loads[1].wait()
    loads[2].wait()
    swap = selection((64, 128), [(0, 0, 64), (32, 64, 32), (0, 96, 32)])
    rope = turned(dot(xr[...], swap), s)
    folded = jnp.where(low_lanes, rope[: ROWS // 2], rope[ROWS // 2 :]).astype(BF16)
    for i in range(4):
        msg[s, ROWS:KV_ROWS, 128 * i : 128 * (i + 1)] = folded[16 * i : 16 * (i + 1)]
    loads[3].wait()
    msg[s, KV_ROWS:, :] = normalized(xq[...], qg_ref[...])

    loads[4].wait()
    left_half = selection((64, 128), [(0, 0, 64)])
    right_half = selection((64, 128), [(0, 64, 64)])

    def folded_weight(w):
        return (dot(w[:256], left_half) + dot(w[256:], right_half)).astype(BF16)

    if spread:
        third = lax.rem(x + s, NX)
        carries = third < 3
        own_third = lax.rem(third, 3)
        is_source = carries & (dp == 3 * s + third)

        @pl.when(is_source)
        def _():
            ws[own_third] = folded_weight(xw[...])

    else:
        for i in range(3):
            ws[i] = folded_weight(xw[:, 64 * i : 64 * (i + 1)])

    pl.semaphore_wait(barrier, greeted)

    part_rows = ((0, KV_ROWS), (KV_ROWS, MSG_ROWS))
    half_rows = (((0, CUT), (KV_ROWS, KV_ROWS + 64)), ((CUT, KV_ROWS), (KV_ROWS + 64, MSG_ROWS)))

    def ring_copy(direction, step, part):
        slot = lax.rem(s + SP - 2 * step, SP) if direction == 0 else lax.rem(s + 2 * step, SP)
        lo, hi = part_rows[part] if step < 3 else half_rows[direction][part]
        piece = msg.at[slot, pl.ds(lo, hi - lo), :]
        return pltpu.make_async_remote_copy(
            src_ref=piece,
            dst_ref=piece,
            send_sem=ring_send.at[direction, step, part],
            recv_sem=ring_recv.at[direction, step, part],
            device_id={"sp": right if direction == 0 else left},
            device_id_type=MESH,
        )

    def ring_arrival(direction, step, part):
        slot = lax.rem(s + SP - 2 * step, SP) if direction == 0 else lax.rem(s + 2 * step, SP)
        lo, hi = part_rows[part] if step < 4 else half_rows[direction][part]
        piece = msg.at[slot, pl.ds(lo, hi - lo), :]
        return pltpu.make_async_remote_copy(
            src_ref=piece,
            dst_ref=piece,
            send_sem=ring_send.at[direction, step - 1, part],
            recv_sem=ring_recv.at[direction, step - 1, part],
            device_id={"sp": right if direction == 0 else left},
            device_id_type=MESH,
        )

    def item_of(direction, step):
        if step == 0:
            return 0
        return 1 + 3 * direction + step - 1 if step < 4 else 7 + direction

    def sib_copy(direction, step, part, mine=True):
        base = s if mine else sib
        slot = lax.rem(base + SP - 2 * step, SP) if direction == 0 else lax.rem(base + 2 * step, SP)
        lo, hi = part_rows[part] if step < 4 else half_rows[direction][part]
        piece = msg.at[slot, pl.ds(lo, hi - lo), :]
        item = item_of(direction, step)
        return pltpu.make_async_remote_copy(
            src_ref=piece,
            dst_ref=piece,
            send_sem=sib_send.at[item, part],
            recv_sem=sib_recv.at[item, part],
            device_id={"sp": sib},
            device_id_type=MESH,
        )

    sends = []

    def start(copy):
        copy.start()
        sends.append(copy)

    for part in range(2):
        for direction in range(2):
            start(ring_copy(direction, 0, part))
        start(sib_copy(0, 0, part))

    def z_copy(step):
        return pltpu.make_async_remote_copy(
            src_ref=ws.at[own_third],
            dst_ref=ws.at[own_third],
            send_sem=wz_send.at[step - 1],
            recv_sem=w_recv.at[own_third],
            device_id={"dp": lax.rem(z + step, nz) * NX + x},
            device_id_type=MESH,
        )

    def x_copy(step):
        return pltpu.make_async_remote_copy(
            src_ref=ws.at[own_third],
            dst_ref=ws.at[own_third],
            send_sem=wx_send.at[step - 1],
            recv_sem=w_recv.at[own_third],
            device_id={"dp": z * NX + lax.rem(x + step, NX)},
            device_id_type=MESH,
        )

    def w_arrival(i):
        return pltpu.make_async_remote_copy(
            src_ref=ws.at[i],
            dst_ref=ws.at[i],
            send_sem=wx_send.at[0],
            recv_sem=w_recv.at[i],
            device_id={"sp": sib},
            device_id_type=MESH,
        )

    if spread:

        @pl.when(is_source)
        def _():
            for step in (6, 5, 7, 4, 8, 3, 9, 2, 10, 1, 11):
                z_copy(step).start()

    def project(slot):
        keyval = dot(msg[slot, 0:ROWS, :], wkv[...])
        at = pl.ds(pl.multiple_of(slot * ROWS, ROWS), ROWS)
        kx[at, 0:NOPE] = keyval[:, :NOPE].astype(BF16)
        vx[at, :] = keyval[:, NOPE:].astype(BF16)
        rope_tile = jnp.concatenate(
            [msg[slot, ROWS:KV_ROWS, 128 * i : 128 * (i + 1)] for i in range(4)], axis=0
        ).astype(F32)
        upper = pl.ds(pl.multiple_of(slot * ROWS, ROWS), ROWS // 2)
        lower = pl.ds(pl.multiple_of(slot * ROWS + ROWS // 2, ROWS // 2), ROWS // 2)
        kx[upper, NOPE:] = jnp.where(low_lanes, rope_tile, 0.0).astype(BF16)
        kx[lower, NOPE:] = jnp.where(low_lanes, 0.0, rope_tile).astype(BF16)

    loads[5].wait()
    project(s)
    sib_copy(0, 0, 0, mine=False).wait_recv()
    project(sib)

    for step in range(1, 5):
        for part in range(2):
            for direction in range(2):
                ring_arrival(direction, step, part).wait_recv()
                if step < 4:
                    start(ring_copy(direction, step, part))
                start(sib_copy(direction, step, part))
            if part == 0 and step < 4:
                for direction in range(2):
                    project(
                        lax.rem(s + SP - 2 * step, SP)
                        if direction == 0
                        else lax.rem(s + 2 * step, SP)
                    )
                    sib_copy(direction, step, part, mine=False).wait_recv()
                    project(
                        lax.rem(sib + SP - 2 * step, SP)
                        if direction == 0
                        else lax.rem(sib + 2 * step, SP)
                    )
            if part == 0 and step == 4:
                project(lax.rem(s + SP // 2, SP))
                for direction in range(2):
                    sib_copy(direction, step, part, mine=False).wait_recv()
                project(lax.rem(sib + SP // 2, SP))
        if step == 2 and spread:

            @pl.when(carries)
            def _():
                @pl.when(jnp.logical_not(is_source))
                def _():
                    w_arrival(own_third).wait_recv()

                for hop in range(1, NX):
                    x_copy(hop).start()

        if step == 3:
            if spread:
                for i in range(3):

                    @pl.when(jnp.logical_or(jnp.logical_not(carries), own_third != i))
                    def _():
                        w_arrival(i).wait_recv()

            take = [
                selection((128, 256), [(0, 0, 64)]),
                selection((128, 256), [(0, 64, 64)]),
                selection((128, 256), [(0, 128, 64), (32, 192, 32), (0, 224, 32)]),
                selection((128, 256), [(64, 0, 64)]),
                selection((128, 256), [(64, 64, 64)]),
                selection((128, 256), [(64, 128, 64), (96, 192, 32), (64, 224, 32)]),
            ]
            for half in range(2):
                wext[256 * half : 256 * (half + 1), :] = (
                    dot(ws[0], take[3 * half])
                    + dot(ws[1], take[3 * half + 1])
                    + dot(ws[2], take[3 * half + 2])
                ).astype(BF16)

    for step in range(5):
        for direction in range(2):
            if step > 0 or direction == 0:
                sib_copy(direction, step, 1, mine=False).wait_recv()

    def ret_copy(target):
        return pltpu.make_async_remote_copy(
            src_ref=att.at[target],
            dst_ref=rcv.at[s],
            send_sem=ret_send.at[target],
            recv_sem=ret_recv.at[s],
            device_id={"sp": target},
            device_id_type=MESH,
        )

    def ret_arrival(source):
        return pltpu.make_async_remote_copy(
            src_ref=att.at[source],
            dst_ref=rcv.at[source],
            send_sem=ret_send.at[source],
            recv_sem=ret_recv.at[source],
            device_id={"sp": sib},
            device_id_type=MESH,
        )

    def away(i):
        order = (0, 3, 5, 4, 2, 6, 1, 7)
        value = order[7]
        for n in range(6, -1, -1):
            value = jnp.where(i == n, order[n], value)
        return value

    def attend(chip, reach):
        rows = 2 * ROWS
        raw = dot(msg[pl.ds(2 * chip, 2), KV_ROWS:, :].reshape(rows, LAT), wext[...])
        rotary = jnp.concatenate(
            [
                turned(raw[:ROWS, NOPE:], 2 * chip),
                turned(raw[ROWS:, NOPE:], 2 * chip + 1),
            ],
            axis=0,
        )
        query = jnp.concatenate([raw[:, :NOPE].astype(BF16), rotary.astype(BF16)], axis=1)
        stop = 512 * (reach + 1)
        scores = lax.dot_general(
            query, kx[0:stop, :], (((1,), (1,)), ((), ())), preferred_element_type=F32
        )
        position = chip * rows + lax.broadcasted_iota(jnp.int32, (rows, 512), 0)
        key = stop - 512 + lax.broadcasted_iota(jnp.int32, (rows, 512), 1)
        last = jnp.where(key <= position, scores[:, stop - 512 :], -jnp.inf)
        top = jnp.max(last, axis=-1, keepdims=True)
        if reach > 0:
            top = jnp.maximum(top, jnp.max(scores[:, : stop - 512], axis=-1, keepdims=True))
        weight = jnp.exp2((last - top) * EXPONENT)
        total = jnp.sum(weight, axis=-1, keepdims=True)
        summed = dot(weight.astype(BF16), vx[stop - 512 : stop, :])
        if reach > 0:
            weight = jnp.exp2((scores[:, : stop - 512] - top) * EXPONENT)
            total = total + jnp.sum(weight, axis=-1, keepdims=True)
            summed = summed + dot(weight.astype(BF16), vx[0 : stop - 512, :])
        attended = (summed / total).astype(BF16)
        att[2 * chip] = attended[:ROWS]
        att[2 * chip + 1] = attended[ROWS:]

    def attend_step(i, carry):
        chip = lax.rem(y + away(i), CHIPS)
        for reach in range(4):

            @pl.when(chip // 2 == reach)
            def _():
                attend(chip, reach)

        @pl.when(i == 0)
        def _():
            rcv[s] = att[s]
            ret_copy(sib).start()

        @pl.when(i > 0)
        def _():
            ret_copy(2 * chip).start()
            ret_copy(2 * chip + 1).start()

        return carry

    lax.fori_loop(0, CHIPS, attend_step, 0)

    acc[...] = jnp.zeros_like(acc)
    ogain[...] = og_ref[...].astype(F32)
    loads[6].wait()

    def out_step(i, squares):
        chip = lax.rem(y + CHIPS - away(i), CHIPS)
        for core in range(2):

            @pl.when(2 * chip + core != s)
            def _():
                ret_arrival(2 * chip + core).wait_recv()

        heads = jnp.concatenate([rcv[2 * chip], rcv[2 * chip + 1]], axis=1).astype(F32)
        gained = (heads * ogain[pl.ds(chip, 1), :]).astype(BF16)
        acc[...] += dot(gained, wout[pl.ds(pl.multiple_of(chip * 256, 256), 256), :])
        return squares + jnp.sum(heads * heads, axis=-1, keepdims=True)

    squares = lax.fori_loop(0, CHIPS, out_step, jnp.zeros((ROWS, 1), F32))
    outv[...] = (acc[...] * lax.rsqrt(squares * (1.0 / D) + EPS)).astype(BF16)
    store = pltpu.make_async_copy(outv, out_ref, load_sem.at[7])
    store.start()

    for copy in sends:
        copy.wait_send()
    for step in range(1, SP):
        ret_copy(lax.rem(s + step, SP)).wait_send()
    if spread:

        @pl.when(is_source)
        def _():
            for step in range(1, nz):
                z_copy(step).wait_send()

        @pl.when(carries)
        def _():
            for hop in range(1, NX):
                x_copy(hop).wait_send()

    store.wait()


def per_device(
    nz, q_latent, kv_latent, rope_key, w_query, w_keyval, w_out, query_gain, latent_gain, out_gain
):
    anywhere = pl.BlockSpec(memory_space=pl.ANY)
    local = pl.BlockSpec(memory_space=pltpu.VMEM)
    dma = pltpu.SemaphoreType.DMA
    result = pl.pallas_call(
        functools.partial(kernel, nz),
        out_shape=jax.ShapeDtypeStruct((ROWS, D), BF16),
        in_specs=[anywhere] * 6 + [local] * 3 + [anywhere],
        out_specs=anywhere,
        scratch_shapes=[
            pltpu.VMEM((ROWS, LAT), BF16),
            pltpu.VMEM((ROWS, LAT), BF16),
            pltpu.VMEM((ROWS, ROPE), BF16),
            pltpu.VMEM(w_query.shape, BF16),
            pltpu.VMEM((LAT, NOPE + VDIM), BF16),
            pltpu.VMEM((H * VDIM, D), BF16),
            pltpu.VMEM((2 * SP + 2 * ROWS, 128), F32),
            pltpu.VMEM((SP, MSG_ROWS, LAT), BF16),
            pltpu.VMEM((3, 256, 128), BF16),
            pltpu.VMEM((LAT, 256), BF16),
            pltpu.VMEM((SP * ROWS, 256), BF16),
            pltpu.VMEM((SP * ROWS, VDIM), BF16),
            pltpu.VMEM((SP, ROWS, VDIM), BF16),
            pltpu.VMEM((SP, ROWS, VDIM), BF16),
            pltpu.VMEM((ROWS, D), F32),
            pltpu.VMEM((ROWS, D), BF16),
            pltpu.VMEM((CHIPS, 256), F32),
            dma((8,)),
            dma((2, 4, 2)),
            dma((2, 4, 2)),
            dma((9, 2)),
            dma((9, 2)),
            dma((SP,)),
            dma((SP,)),
            dma((11,)),
            dma((3,)),
            dma((3,)),
        ],
        compiler_params=pltpu.CompilerParams(
            collective_id=0, has_side_effects=True, vmem_limit_bytes=60 * 1024 * 1024
        ),
    )(
        q_latent[0],
        kv_latent[0],
        rope_key[0],
        w_query,
        w_keyval,
        w_out,
        query_gain.reshape(1, LAT),
        latent_gain.reshape(1, LAT),
        out_gain.reshape(CHIPS, 256),
        jnp.asarray(rotary_tables()),
    )
    return result[None]


def solution(mesh):
    nz = mesh.shape["dp"] // NX
    rows = P("dp", "sp", None)
    return jax.shard_map(
        functools.partial(per_device, nz),
        mesh=mesh,
        in_specs=(rows, rows, rows, P(None, "dp"), P(None, "sp"), P(), P(), P(), P()),
        out_specs=rows,
        check_vma=False,
    )
```
